512 devices in a mesh: kv: 128 (over z, y, core), tp: 4 (over x).
Axes of the slice: x: 4, y: 8, z: 8, core: 2. Of those that a mesh axis runs over, the one named last changes fastest.
Arguments:
- tokens: bfloat16 [8, 2048], P(None, 'kv'), may hold values from -6 to 6
- in_gain: float32 [2048], P('kv'), may hold values from 0.1 to 1.9
- w_query: bfloat16 [2048, 512], P('kv', 'tp'), may hold values from -0.125 to 0.125
- score_bias: float32 [4], P('tp'), as said below
- cache_keys: bfloat16 [8, 131072, 512], P(None, 'kv', 'tp'), may hold values from -8 to 8, as said below
- cache_values: bfloat16 [8, 131072, 512], P(None, 'kv', 'tp'), may hold values from -6 to 6
- lengths: int32 [8], replicated, may hold values from 16384 to 131072, as said below
- head_gain: float32 [512], P('tp'), may hold values from 0.1 to 1.9
- w_out: bfloat16 [512, 2048], P('tp', 'kv'), may hold values from -0.25 to 0.25
Outputs:
- mixed: bfloat16 [8, 2048], P(None, 'kv')
The draws below stay inside these ranges and needn't reach their ends.
Inputs may be any that keep to these rules, and one draw needn't show every extreme that they name: `score_bias`: one value a head, added to every score of that head. `cache_keys`: real-valued key entries. `lengths`: one sequence has all 131072 positions cached.
All inputs are finite; a program needn't handle non-finite values.
Results may differ from the reference program's by a relative error of at most 0.0095.
The reference program's roundings to bfloat16 on the way (of `gained`, `queries`, `weights` and `normed`) count: a program that leaves them out, or rounds other values in their place, can miss the bound.
Values may be sent and summed in bfloat16 or wider, within the bound.
A program may use at most 64 MiB of HBM per device.

```python
import jax
import jax.numpy as jnp
from jax import lax

D = 2048
HEADS = 4
DH = 128
SEQS = 8
POS_DEV = 1024
SEQ_LEN = 131072
N_TP = 4


def draw_score_bias(key, part):
    key_order, key_slow, key_fast = jax.random.split(jax.random.fold_in(key, 11), 3)
    slow_heads = jax.random.permutation(key_order, HEADS) < HEADS // 2
    slow_value = -jnp.log(jnp.float32(SEQ_LEN)) + jax.random.uniform(key_slow, (HEADS,), jnp.float32, -0.6, 0.0)
    fast_value = -jnp.log(jax.random.uniform(key_fast, (HEADS,), jnp.float32, 30.0, 100.0)) - 1.1
    return jnp.where(slow_heads, slow_value, fast_value).astype(jnp.float32)


def draw_cache_keys(key, part):
    key_scale, key_base = jax.random.split(jax.random.fold_in(key, 3))
    spans = SEQ_LEN // 32
    span_scale = jax.random.uniform(key_scale, (SEQS, spans, 1, HEADS, 1), jnp.float32, 0.5, 2.0)
    unit_draw = jnp.clip(jax.random.normal(key_base, (SEQS, spans, 32, HEADS, DH), jnp.float32), -4.0, 4.0)
    return (unit_draw * span_scale).reshape(SEQS, SEQ_LEN, HEADS * DH).astype(jnp.bfloat16)


def draw_lengths(key, part):
    key_lens, key_full = jax.random.split(jax.random.fold_in(key, 7))
    drawn = jax.random.randint(key_lens, (SEQS,), SEQ_LEN // 8, SEQ_LEN + 1)
    chosen = jax.random.randint(key_full, (), 0, SEQS)
    return jnp.where(jnp.arange(SEQS) == chosen, SEQ_LEN, drawn).astype(jnp.int32)


def level_of(rng, dims, cuts, least, largest):
    level, own = 1.0, jax.random.fold_in(rng, 6)
    for dim, parts in cuts:
        heights = jnp.exp(jax.random.uniform(jax.random.fold_in(own, dim), (parts,), jnp.float32, least / len(cuts), largest / len(cuts)))
        level = level * jnp.repeat(heights, dims[dim] // parts).reshape([-1 if axis == dim else 1 for axis in range(len(dims))])
    return level


def bell_draw(stream_key, extent, deviation, reach, shards=(), kind=jnp.bfloat16):
    values = deviation * jax.random.normal(stream_key, extent, jnp.float32)
    if shards:
        values = values * level_of(stream_key, extent, shards, -0.22, 0.18)
    return jnp.clip(values, -reach, reach).astype(kind)


def setup_inputs(seed: int = 0) -> dict:
    key_of = jax.random.split(jax.random.key(seed), 10)
    tokens = bell_draw(key_of[0], (SEQS, D), 1.0, 6.0, ((1, 128),))
    in_gain = jnp.clip(1.0 + 0.18 * jax.random.normal(key_of[1], (D,), jnp.float32), 0.1, 1.9)
    w_query = bell_draw(key_of[2], (D, HEADS * DH), D ** -0.5, 0.125, ((0, 128), (1, 4)))
    score_bias = draw_score_bias(jax.random.fold_in(key_of[9], 71), 0)
    cache_keys = draw_cache_keys(jax.random.fold_in(key_of[9], 71), 0)
    cache_values = bell_draw(key_of[5], (SEQS, SEQ_LEN, HEADS * DH), 1.0, 6.0, ((1, 128), (2, 4)))
    lengths = draw_lengths(jax.random.fold_in(key_of[9], 71), 0)
    head_gain = jnp.clip(1.0 + 0.18 * jax.random.normal(key_of[7], (HEADS * DH,), jnp.float32), 0.1, 1.9)
    w_out = bell_draw(key_of[8], (HEADS * DH, D), (HEADS * DH) ** -0.5, 0.25, ((0, 4), (1, 128)))
    return dict(tokens=tokens, in_gain=in_gain, w_query=w_query, score_bias=score_bias, cache_keys=cache_keys, cache_values=cache_values, lengths=lengths, head_gain=head_gain, w_out=w_out)


EPS = 1e-06

def reference(tokens, in_gain, w_query, score_bias, cache_keys, cache_values, lengths, head_gain, w_out):
    as_float = tokens.astype(jnp.float32)
    gained = (as_float * in_gain).astype(jnp.bfloat16)
    raw_query = jnp.dot(gained, w_query, preferred_element_type=jnp.float32)
    row_scale = lax.rsqrt(lax.optimization_barrier(jnp.mean(as_float * as_float, axis=1)) + EPS)
    queries = (raw_query * row_scale[:, None]).astype(jnp.bfloat16).reshape(SEQS, HEADS, DH)
    segments = SEQ_LEN // POS_DEV

    def per_sequence(fields):
        seq_query, seq_keys, seq_values, seq_len = fields
        keys_f32 = seq_keys.astype(jnp.float32).reshape(SEQ_LEN, HEADS, DH)
        scores = jnp.einsum('hd,lhd->hl', seq_query.astype(jnp.float32), keys_f32) * DH ** (-0.5)
        scores = scores + score_bias[:, None]
        usable = (jnp.arange(SEQ_LEN, dtype=jnp.int32) < seq_len)[None, :]
        log_keep = jnp.where(usable, jax.nn.log_sigmoid(-scores), 0.0)
        segmented = log_keep.reshape(HEADS, segments, POS_DEV)
        suffix = lax.cumsum(segmented, axis=2, reverse=True) - segmented
        gate_log = jax.nn.log_sigmoid(scores).reshape(HEADS, segments, POS_DEV)
        weights = jnp.where(usable.reshape(1, segments, POS_DEV), jnp.exp(gate_log + suffix), 0.0)
        weights = weights.astype(jnp.bfloat16)
        values_f32 = seq_values.astype(jnp.float32).reshape(segments, POS_DEV, HEADS, DH)
        seg_out = jnp.einsum('hnp,nphd->hnd', weights.astype(jnp.float32), values_f32)
        totals = lax.optimization_barrier(jnp.sum(segmented, axis=2))
        later_sum = lax.cumsum(totals, axis=1, reverse=True) - totals
        return lax.optimization_barrier(jnp.sum(seg_out * jnp.exp(later_sum)[..., None], axis=1))
    attended = lax.map(per_sequence, (queries, cache_keys, cache_values, lengths))
    mean_sq = lax.optimization_barrier(jnp.mean(attended * attended, axis=2))
    normed = attended * lax.rsqrt(mean_sq + EPS)[..., None]
    normed = (normed.reshape(SEQS, HEADS * DH) * head_gain).astype(jnp.bfloat16)
    block_width = HEADS * DH // N_TP
    mixed = jnp.zeros((SEQS, D), jnp.float32)
    for block in range(N_TP):
        part_out = jnp.dot(normed[:, block * block_width:(block + 1) * block_width], w_out[block * block_width:(block + 1) * block_width], preferred_element_type=jnp.float32)
        mixed = mixed + lax.optimization_barrier(part_out.astype(jnp.bfloat16)).astype(jnp.float32)
    return mixed.astype(jnp.bfloat16)
```

```python
import functools

import jax
import jax.numpy as jnp
from jax import lax
from jax.experimental import pallas as pl
from jax.experimental.pallas import tpu as pltpu
from jax.sharding import PartitionSpec as P

MESH = pl.DeviceIdType.MESH
D = 2048
EPS = 1e-06
SEQS = 8
DH = 128
SEG = 1024
CHUNKS = SEG // 128
RING = 8
OFFSETS = (4, 3, 5, 2, 6, 1, 7, 0)
F32 = jnp.float32
BF16 = jnp.bfloat16


def kernel(
    tokens_hbm, gain_hbm, wq_hbm, bias_ref, keys_hbm, values_hbm, lengths_ref, head_gain_hbm, wout_hbm,
    out_ref,
    tokens_v, gain_v, wq_v, keys_v, values_v, head_gain_v, wout_v,
    send_a1, recv_a1, recv_a2, send_b1, recv_b1, recv_b2, recv_c,
    load_sems, key_sems, value_sems,
    a1_s, a1_r, a2_s, a2_r, b1_s, b1_r, b2_s, b2_r, c_s, c_r,
):
    kv = lax.axis_index("kv")
    tp = lax.axis_index("tp")
    z, y, core = kv // 16, (kv // 2) % 8, kv % 2

    def at(zz, yy, cc, xx):
        return {"kv": (zz * 8 + yy) * 2 + cc, "tp": xx}

    y_peers = [(2 * dy + dc, (y + dy) % 8, (core + dc) % 2) for dy in OFFSETS for dc in (0, 1) if dy or dc]
    z_peers = [(2 * dz + dc, (z + dz) % 8, (core + dc) % 2) for dz in OFFSETS for dc in (0, 1) if dz or dc]

    barrier = pltpu.get_barrier_semaphore()
    for k, yy, cc in y_peers:
        pl.semaphore_signal(barrier, inc=1, device_id=at(z, yy, cc, tp), device_id_type=MESH)
    for k, zz, cc in z_peers:
        if k > 1:
            pl.semaphore_signal(barrier, inc=1, device_id=at(zz, y, cc, tp), device_id_type=MESH)
    for dx in (2, 1, 3):
        pl.semaphore_signal(barrier, inc=1, device_id=at(z, y, core, (tp + dx) % 4), device_id_type=MESH)

    small = [
        pltpu.make_async_copy(src, dst, load_sems.at[i])
        for i, (src, dst) in enumerate(
            [(tokens_hbm, tokens_v), (gain_hbm, gain_v), (wq_hbm, wq_v), (head_gain_hbm, head_gain_v), (wout_hbm, wout_v)]
        )
    ]
    for copy in small:
        copy.start()
    key_copies = [pltpu.make_async_copy(keys_hbm.at[b], keys_v.at[b], key_sems.at[b]) for b in range(SEQS)]
    value_copies = [pltpu.make_async_copy(values_hbm.at[b], values_v.at[b], value_sems.at[b]) for b in range(SEQS)]
    for copy in key_copies + value_copies:
        copy.start()

    row = lax.broadcasted_iota(jnp.int32, (8, 128), 0)
    upper = row < 4

    def swap(tile):
        return pltpu.roll(tile, 4, 0)

    def halves(full, scalars):
        return jnp.where(upper, full, swap(scalars)), jnp.where(upper, swap(full), scalars)

    def joined(first, second):
        return jnp.where(upper, first, swap(second)), jnp.where(upper, swap(first), second)

    def scatter_y(src, dst, s_sems, r_sems):
        copies = []
        for k, yy, cc in y_peers:
            copies.append(
                pltpu.make_async_remote_copy(
                    src_ref=src.at[cc], dst_ref=dst.at[y * 2 + core], send_sem=s_sems.at[k], recv_sem=r_sems.at[k],
                    device_id=at(z, yy, cc, tp), device_id_type=MESH,
                )
            )
            copies[-1].start()
        return copies

    def spread_z(dst, s_sems, r_sems):
        copies = []
        for k, zz, cc in z_peers:
            copies.append(
                pltpu.make_async_remote_copy(
                    src_ref=dst.at[z * 2 + core], dst_ref=dst.at[z * 2 + core], send_sem=s_sems.at[k],
                    recv_sem=r_sems.at[k], device_id=at(zz, y, cc, tp), device_id_type=MESH,
                )
            )
            copies[-1].start()
        return copies

    for copy in small[:3]:
        copy.wait()
    as_float = tokens_v[...].astype(F32)
    gained = (as_float * gain_v[...]).astype(BF16)
    partial = jnp.dot(gained, wq_v[...], preferred_element_type=F32)
    squares = jnp.broadcast_to(jnp.sum(as_float * as_float, axis=1, keepdims=True), (8, 128))
    first, second = halves(partial, squares)
    send_a1[0] = first
    send_a1[1] = second
    recv_a1[y * 2 + core] = jnp.where(core == 0, first, second)
    pl.semaphore_wait(barrier, 32)
    copies_a1 = scatter_y(send_a1, recv_a1, a1_s, a1_r)
    for copy in copies_a1:
        copy.wait_recv()
    recv_a2[z * 2 + core] = jnp.sum(recv_a1[...], axis=0)
    copies_a2 = spread_z(recv_a2, a2_s, a2_r)

    r_iota = lax.broadcasted_iota(jnp.int32, (128, 256), 0)
    s_iota = lax.broadcasted_iota(jnp.int32, (128, 256), 1)
    after = jnp.where((r_iota > s_iota) | (s_iota >= 128), 1.0, 0.0).astype(BF16)
    length = jnp.zeros((8, 128), jnp.int32)
    for b in range(SEQS):
        length = jnp.where(row == b, lengths_ref[b], length)
    bias = bias_ref[0]
    for copy in key_copies:
        copy.wait()

    for copy in copies_a2:
        copy.wait_recv()
    by_core = jnp.sum(recv_a2[...].reshape(8, 2, 8, 128), axis=0)
    summed, total_sq = joined(by_core[0], by_core[1])
    query = (summed * lax.rsqrt(total_sq / D + EPS)).astype(BF16)

    dims = (((1,), (1,)), ((), ()))
    raw = [None] * CHUNKS
    for b in range(SEQS):
        got = lax.dot_general(query, keys_v[b], dims, preferred_element_type=F32)
        for n in range(CHUNKS):
            piece = got[:, n * 128 : (n + 1) * 128]
            raw[n] = piece if b == 0 else jnp.where(row == b, piece, raw[n])
    lane = lax.broadcasted_iota(jnp.int32, (8, 128), 1)
    log_gate, log_keep, usable = [], [], []
    for n in range(CHUNKS):
        score = raw[n] * DH**-0.5 + bias
        tail = jnp.log1p(jnp.exp(-jnp.abs(score)))
        ok = lane + (kv * SEG + n * 128) < length
        usable.append(ok)
        log_gate.append(jnp.minimum(score, 0.0) - tail)
        log_keep.append(jnp.where(ok, -jnp.maximum(score, 0.0) - tail, 0.0))
    keep = jnp.concatenate(log_keep, axis=0)
    high = keep.astype(BF16)
    rest = keep - high.astype(F32)
    mid = rest.astype(BF16)
    low = (rest - mid.astype(F32)).astype(BF16)
    sums = jnp.dot(jnp.concatenate([high, mid, low], axis=0), after, preferred_element_type=F32)
    sums = sums[0:64] + sums[64:128] + sums[128:192]
    later = jnp.zeros((8, 128), F32)
    pieces = [None] * CHUNKS
    for n in reversed(range(CHUNKS)):
        inside = sums[n * 8 : n * 8 + 8, 0:128]
        pieces[n] = jnp.where(usable[n], jnp.exp(log_gate[n] + (inside + later)), 0.0).astype(BF16)
        later = later + sums[n * 8 : n * 8 + 8, 128:256]
    weights = jnp.concatenate(pieces, axis=1)
    for copy in value_copies:
        copy.wait()
    local = None
    for b in range(SEQS):
        got = jnp.dot(weights, values_v[b], preferred_element_type=F32)
        local = got if b == 0 else jnp.where(row == b, got, local)

    first, second = halves(local, later)
    send_b1[0] = first
    send_b1[1] = second
    recv_b1[y * 2 + core] = jnp.where(core == 0, first, second)
    copies_b1 = scatter_y(send_b1, recv_b1, b1_s, b1_r)
    for copy in copies_b1:
        copy.wait_recv()
    later = jnp.zeros((8, 128), F32)
    total = jnp.zeros((8, 128), F32)
    for i in reversed(range(16)):
        tile = recv_b1[i]
        total = total + tile * jnp.exp(swap(jnp.where(upper, 0.0, later)))
        later = later + tile
    recv_b2[z * 2 + core] = jnp.where(upper, total, later)
    copies_b2 = spread_z(recv_b2, b2_s, b2_r)
    for copy in small[3:]:
        copy.wait()
    for copy in copies_b2:
        copy.wait_recv()
    later = jnp.zeros((8, 128), F32)
    attended = jnp.zeros((8, 128), F32)
    for i in reversed(range(8)):
        outs, totals = joined(recv_b2[2 * i], recv_b2[2 * i + 1])
        attended = attended + outs * jnp.exp(later)
        later = later + totals

    mean_sq = jnp.sum(attended * attended, axis=1, keepdims=True) / DH
    normed = (attended * lax.rsqrt(mean_sq + EPS) * head_gain_v[...]).astype(BF16)
    part = lax.dot_general(normed, wout_v[...], dims, preferred_element_type=F32)
    recv_c[tp] = part.astype(BF16)
    copies_c = []
    for k, dx in enumerate((2, 1, 3)):
        copies_c.append(
            pltpu.make_async_remote_copy(
                src_ref=recv_c.at[tp], dst_ref=recv_c.at[tp], send_sem=c_s.at[k], recv_sem=c_r.at[k],
                device_id=at(z, y, core, (tp + dx) % 4), device_id_type=MESH,
            )
        )
        copies_c[-1].start()
    for copy in copies_a1 + copies_a2 + copies_b1 + copies_b2:
        copy.wait_send()
    for copy in copies_c:
        copy.wait()
    mixed = recv_c[0].astype(F32)
    for i in range(1, 4):
        mixed = mixed + recv_c[i].astype(F32)
    out_ref[...] = mixed.astype(BF16)


def shards(tokens, in_gain, w_query, score_bias, cache_keys, cache_values, lengths, head_gain, w_out):
    dma = pltpu.SemaphoreType.DMA
    any_space = pl.BlockSpec(memory_space=pl.ANY)
    smem = pl.BlockSpec(memory_space=pltpu.SMEM)
    return pl.pallas_call(
        kernel,
        out_shape=jax.ShapeDtypeStruct((SEQS, 16), BF16),
        in_specs=[any_space, any_space, any_space, smem, any_space, any_space, smem, any_space, any_space],
        out_specs=pl.BlockSpec(memory_space=pltpu.VMEM),
        scratch_shapes=[
            pltpu.VMEM((SEQS, 16), BF16),
            pltpu.VMEM((1, 16), F32),
            pltpu.VMEM((16, DH), BF16),
            pltpu.VMEM((SEQS, SEG, DH), BF16),
            pltpu.VMEM((SEQS, SEG, DH), BF16),
            pltpu.VMEM((1, DH), F32),
            pltpu.VMEM((16, DH), BF16),
            pltpu.VMEM((2, 8, 128), F32),
            pltpu.VMEM((16, 8, 128), F32),
            pltpu.VMEM((16, 8, 128), F32),
            pltpu.VMEM((2, 8, 128), F32),
            pltpu.VMEM((16, 8, 128), F32),
            pltpu.VMEM((16, 8, 128), F32),
            pltpu.VMEM((4, SEQS, 16), BF16),
            dma((5,)),
            dma((SEQS,)),
            dma((SEQS,)),
            dma((16,)),
            dma((16,)),
            dma((16,)),
            dma((16,)),
            dma((16,)),
            dma((16,)),
            dma((16,)),
            dma((16,)),
            dma((3,)),
            dma((3,)),
        ],
        compiler_params=pltpu.CompilerParams(collective_id=0, has_side_effects=True),
        name="decode",
    )(
        tokens, in_gain.reshape(1, 16), w_query, score_bias, cache_keys, cache_values, lengths,
        head_gain.reshape(1, DH), w_out.T,
    )


def solution(mesh):
    placed = (
        P(None, "kv"), P("kv"), P("kv", "tp"), P("tp"), P(None, "kv", "tp"), P(None, "kv", "tp"), P(), P("tp"),
        P("tp", "kv"),
    )
    return jax.shard_map(shards, mesh=mesh, in_specs=placed, out_specs=P(None, "kv"), check_vma=False)
```

```python
import jax
import jax.numpy as jnp
from jax import lax
from jax.experimental import pallas as pl
from jax.experimental.pallas import tpu as pltpu
from jax.sharding import PartitionSpec as P

MESH = pl.DeviceIdType.MESH
D = 2048
EPS = 1e-06
SEQS = 8
DH = 128
SEG = 1024
CHUNKS = SEG // 128
COLS = 16
OFFSETS = (4, 3, 5, 2, 6, 1, 7)
F32 = jnp.float32
BF16 = jnp.bfloat16
DIMS = (((1,), (1,)), ((), ()))


def kernel(
    tokens_hbm, gain_hbm, wq_hbm, bias_ref, keys_hbm, values_hbm, lengths_ref, head_gain_hbm, wout_hbm,
    out_ref,
    tokens_v, gain_v, wq_v, keys_v, values_v, head_gain_v, wout_v,
    sum_y, sum_z, total_y, total_z, local_y, local_z, parts, parts_0,
    load_sems, key_sems, value_sems, wout_s, wout_r,
    sum_y_s, sum_y_r, sum_z_s, sum_z_r, total_y_s, total_y_r, total_z_s, total_z_r,
    local_y_s, local_y_r, local_z_s, local_z_r, parts_s, parts_r,
):
    kv = lax.axis_index("kv")
    tp = lax.axis_index("tp")
    z, y, core = kv // 16, (kv // 2) % 8, kv % 2
    adder = core == 1
    mine = y * 2 + core

    def at(zz, yy, cc, xx):
        return {"kv": (zz * 8 + yy) * 2 + cc, "tp": xx}

    def signal(zz, yy, cc, xx):
        pl.semaphore_signal(barrier, inc=1, device_id=at(zz, yy, cc, xx), device_id_type=MESH)

    def send(src, dst, s_sem, r_sem, zz, yy, cc, xx):
        copy = pltpu.make_async_remote_copy(
            src_ref=src, dst_ref=dst, send_sem=s_sem, recv_sem=r_sem, device_id=at(zz, yy, cc, xx), device_id_type=MESH
        )
        copy.start()

    def waiter(dst, s_sem, r_sem):
        return pltpu.make_async_remote_copy(
            src_ref=dst, dst_ref=dst, send_sem=s_sem, recv_sem=r_sem, device_id=at(z, y, 1 - core, tp), device_id_type=MESH
        )

    barrier = pltpu.get_barrier_semaphore()

    @pl.when(adder)
    def _():
        for d in OFFSETS:
            for cc in (0, 1):
                signal(z, (y + d) % 8, cc, tp)
            signal((z + d) % 8, y, 1, tp)
        for d in (2, 1, 3):
            signal(z, y, 1, (tp + d) % 4)
        signal(z, y, 0, tp)

    @pl.when(core == 0)
    def _():
        for d in OFFSETS:
            signal((z + d) % 8, y, 1, tp)
        for d in (2, 1, 3):
            signal(z, y, 1, (tp + d) % 4)
        signal(z, y, 1, tp)

    small = [
        pltpu.make_async_copy(src, dst, load_sems.at[i])
        for i, (src, dst) in enumerate(
            [(tokens_hbm, tokens_v), (gain_hbm, gain_v), (wq_hbm, wq_v), (head_gain_hbm, head_gain_v),
             (wout_hbm, wout_v.at[core])]
        )
    ]
    for copy in small:
        copy.start()
    key_copies = [pltpu.make_async_copy(keys_hbm.at[b], keys_v.at[b], key_sems.at[b]) for b in range(SEQS)]
    value_copies = [pltpu.make_async_copy(values_hbm.at[b], values_v.at[b], value_sems.at[b]) for b in range(SEQS)]
    for copy in key_copies + value_copies:
        copy.start()

    row = lax.broadcasted_iota(jnp.int32, (8, 128), 0)
    lane = lax.broadcasted_iota(jnp.int32, (8, 128), 1)

    def to_adders(buf, s_sems, r_sems):
        for d in OFFSETS:
            send(buf.at[mine], buf.at[mine], s_sems.at[d], r_sems.at[2 * ((8 - d) % 8) + core], z, (y + d) % 8, 1, tp)

        @pl.when(core == 0)
        def _():
            send(buf.at[mine], buf.at[mine], s_sems.at[0], r_sems.at[0], z, y, 1, tp)

    def from_line(buf, s_sems, r_sems):
        for d in OFFSETS:
            for cc in (0, 1):
                waiter(buf.at[mine], s_sems.at[0], r_sems.at[2 * d + cc]).wait_recv()
        waiter(buf.at[mine], s_sems.at[0], r_sems.at[0]).wait_recv()

    def sent_to_adders(buf, s_sems, r_sems):
        for d in OFFSETS:
            waiter(buf.at[mine], s_sems.at[d], r_sems.at[0]).wait_send()

        @pl.when(core == 0)
        def _():
            waiter(buf.at[mine], s_sems.at[0], r_sems.at[0]).wait_send()

    for copy in small[:3]:
        copy.wait()
    as_float = tokens_v[...].astype(F32)
    gained = (as_float * gain_v[...]).astype(BF16)
    partial = jnp.dot(gained, wq_v[...], preferred_element_type=F32)
    squares = jnp.sum(as_float * as_float, axis=1, keepdims=True)
    sum_y[mine, 0:8] = partial
    sum_y[mine, 8:9] = jnp.sum(jnp.where(row == lane, squares, 0.0), axis=0, keepdims=True)

    @pl.when(adder)
    def _():
        pl.semaphore_wait(barrier, 28)

    @pl.when(core == 0)
    def _():
        pl.semaphore_wait(barrier, 8)

    to_adders(sum_y, sum_y_s, sum_y_r)

    @pl.when(core == 0)
    def _():
        small[4].wait()
        send(wout_v.at[0], wout_v.at[0], wout_s, wout_r, z, y, 1, tp)

    @pl.when(adder)
    def _():
        from_line(sum_y, sum_y_s, sum_y_r)
        sum_z[z] = jnp.sum(sum_y[...], axis=0)
        for d in OFFSETS:
            for cc in (0, 1):
                send(sum_z.at[z], sum_z.at[z], sum_z_s.at[2 * d + cc], sum_z_r.at[(8 - d) % 8], (z + d) % 8, y, cc, tp)
        send(sum_z.at[z], sum_z.at[z], sum_z_s.at[0], sum_z_r.at[0], z, y, 0, tp)

    r_iota = lax.broadcasted_iota(jnp.int32, (128, 256), 0)
    s_iota = lax.broadcasted_iota(jnp.int32, (128, 256), 1)
    after = jnp.where((r_iota > s_iota) | (s_iota >= 128), 1.0, 0.0).astype(BF16)
    length = jnp.zeros((8, 128), jnp.int32)
    for b in range(SEQS):
        length = jnp.where(row == b, lengths_ref[b], length)
    bias = bias_ref[0]
    for copy in key_copies + value_copies:
        copy.wait()

    for d in OFFSETS:
        waiter(sum_z.at[z], sum_z_s.at[0], sum_z_r.at[d]).wait_recv()

    @pl.when(core == 0)
    def _():
        waiter(sum_z.at[z], sum_z_s.at[0], sum_z_r.at[0]).wait_recv()

    summed = jnp.sum(sum_z[...], axis=0)
    total_sq = jnp.sum(jnp.where(row == lane, summed[8:9], 0.0), axis=1, keepdims=True)
    query = (summed[0:8] * lax.rsqrt(total_sq / D + EPS)).astype(BF16)

    raw = [None] * CHUNKS
    for b in range(SEQS):
        got = lax.dot_general(query, keys_v[b], DIMS, preferred_element_type=F32)
        for n in range(CHUNKS):
            piece = got[:, n * 128 : (n + 1) * 128]
            raw[n] = piece if b == 0 else jnp.where(row == b, piece, raw[n])
    log_gate, log_keep, usable = [], [], []
    for n in range(CHUNKS):
        score = raw[n] * DH**-0.5 + bias
        tail = jnp.log1p(jnp.exp(-jnp.abs(score)))
        ok = lane + (kv * SEG + n * 128) < length
        usable.append(ok)
        log_gate.append(jnp.minimum(score, 0.0) - tail)
        log_keep.append(jnp.where(ok, -jnp.maximum(score, 0.0) - tail, 0.0))
    keep = jnp.concatenate(log_keep, axis=0)
    high = keep.astype(BF16)
    rest = keep - high.astype(F32)
    mid = rest.astype(BF16)
    low = (rest - mid.astype(F32)).astype(BF16)
    sums = jnp.dot(jnp.concatenate([high, mid, low], axis=0), after, preferred_element_type=F32)
    sums = sums[0:64] + sums[64:128] + sums[128:192]
    later = jnp.zeros((8, 128), F32)
    pieces = [None] * CHUNKS
    for n in reversed(range(CHUNKS)):
        inside = sums[n * 8 : n * 8 + 8, 0:128]
        pieces[n] = jnp.where(usable[n], jnp.exp(log_gate[n] + (inside + later)), 0.0).astype(BF16)
        later = later + sums[n * 8 : n * 8 + 8, 128:256]
    total_y[mine] = later
    to_adders(total_y, total_y_s, total_y_r)
    weights = jnp.concatenate(pieces, axis=1)
    local = None
    for b in range(SEQS):
        got = jnp.dot(weights, values_v[b], preferred_element_type=F32)
        local = got if b == 0 else jnp.where(row == b, got, local)
    local_y[mine] = local
    to_adders(local_y, local_y_s, local_y_r)

    @pl.when(adder)
    def _():
        from_line(total_y, total_y_s, total_y_r)
        later = jnp.zeros((8, 128), F32)
        fade = [None] * 16
        for i in reversed(range(16)):
            fade[i] = jnp.exp(later)
            later = later + total_y[i]
        total_z[z] = later
        for d in OFFSETS:
            send(total_z.at[z], total_z.at[z], total_z_s.at[d], total_z_r.at[(8 - d) % 8], (z + d) % 8, y, 1, tp)
        from_line(local_y, local_y_s, local_y_r)
        terms = [local_y[i] * fade[i] for i in range(16)]
        while len(terms) > 1:
            terms = [a + b for a, b in zip(terms[::2], terms[1::2])]
        local_z[z] = terms[0]
        for d in OFFSETS:
            send(local_z.at[z], local_z.at[z], local_z_s.at[d], local_z_r.at[(8 - d) % 8], (z + d) % 8, y, 1, tp)
        for copy in small[3:]:
            copy.wait()
        waiter(wout_v.at[0], wout_s, wout_r).wait_recv()
        for d in OFFSETS:
            waiter(total_z.at[z], total_z_s.at[0], total_z_r.at[d]).wait_recv()
        later = jnp.zeros((8, 128), F32)
        fade = [None] * 8
        for i in reversed(range(8)):
            fade[i] = jnp.exp(later)
            later = later + total_z[i]
        for d in OFFSETS:
            waiter(local_z.at[z], local_z_s.at[0], local_z_r.at[d]).wait_recv()
        terms = [local_z[i] * fade[i] for i in range(8)]
        while len(terms) > 1:
            terms = [a + b for a, b in zip(terms[::2], terms[1::2])]
        attended = terms[0]
        mean_sq = jnp.sum(attended * attended, axis=1, keepdims=True) / DH
        normed = (attended * lax.rsqrt(mean_sq + EPS) * head_gain_v[...]).astype(BF16)
        parts[tp] = lax.dot_general(normed, wout_v[1], DIMS, preferred_element_type=F32).astype(BF16)
        parts_0[...] = lax.dot_general(normed, wout_v[0], DIMS, preferred_element_type=F32).astype(BF16)
        for d in (2, 1, 3):
            send(parts_0, parts.at[tp], parts_s.at[d], parts_r.at[4 - d], z, y, 0, (tp + d) % 4)
            send(parts.at[tp], parts.at[tp], parts_s.at[4 + d], parts_r.at[4 - d], z, y, 1, (tp + d) % 4)
        send(parts_0, parts.at[tp], parts_s.at[0], parts_r.at[0], z, y, 0, tp)

    sent_to_adders(sum_y, sum_y_s, sum_y_r)
    sent_to_adders(total_y, total_y_s, total_y_r)
    sent_to_adders(local_y, local_y_s, local_y_r)

    @pl.when(adder)
    def _():
        for d in OFFSETS:
            for cc in (0, 1):
                waiter(sum_z.at[z], sum_z_s.at[2 * d + cc], sum_z_r.at[0]).wait_send()
            waiter(total_z.at[z], total_z_s.at[d], total_z_r.at[0]).wait_send()
            waiter(local_z.at[z], local_z_s.at[d], local_z_r.at[0]).wait_send()
        waiter(sum_z.at[z], sum_z_s.at[0], sum_z_r.at[0]).wait_send()
        for d in (2, 1, 3):
            for first in (0, 4):
                waiter(parts.at[tp], parts_s.at[first + d], parts_r.at[0]).wait_send()
        waiter(parts.at[tp], parts_s.at[0], parts_r.at[0]).wait_send()

    @pl.when(core == 0)
    def _():
        waiter(wout_v.at[0], wout_s, wout_r).wait_send()
        small[3].wait()
        waiter(parts.at[tp], parts_s.at[0], parts_r.at[0]).wait_recv()

    for d in (2, 1, 3):
        waiter(parts.at[tp], parts_s.at[0], parts_r.at[d]).wait_recv()
    mixed = parts[0].astype(F32)
    for i in range(1, 4):
        mixed = mixed + parts[i].astype(F32)
    out_ref[...] = mixed.astype(BF16)


def shards(tokens, in_gain, w_query, score_bias, cache_keys, cache_values, lengths, head_gain, w_out):
    dma = pltpu.SemaphoreType.DMA
    any_space = pl.BlockSpec(memory_space=pl.ANY)
    smem = pl.BlockSpec(memory_space=pltpu.SMEM)
    return pl.pallas_call(
        kernel,
        out_shape=jax.ShapeDtypeStruct((SEQS, COLS), BF16),
        in_specs=[any_space, any_space, any_space, smem, any_space, any_space, smem, any_space, any_space],
        out_specs=pl.BlockSpec(memory_space=pltpu.VMEM),
        scratch_shapes=[
            pltpu.VMEM((SEQS, 16), BF16),
            pltpu.VMEM((1, 16), F32),
            pltpu.VMEM((16, DH), BF16),
            pltpu.VMEM((SEQS, SEG, DH), BF16),
            pltpu.VMEM((SEQS, SEG, DH), BF16),
            pltpu.VMEM((1, DH), F32),
            pltpu.VMEM((2, COLS, DH), BF16),
            pltpu.VMEM((16, 9, 128), F32),
            pltpu.VMEM((8, 9, 128), F32),
            pltpu.VMEM((16, 8, 128), F32),
            pltpu.VMEM((8, 8, 128), F32),
            pltpu.VMEM((16, 8, 128), F32),
            pltpu.VMEM((8, 8, 128), F32),
            pltpu.VMEM((4, SEQS, COLS), BF16),
            pltpu.VMEM((SEQS, COLS), BF16),
            dma((5,)),
            dma((SEQS,)),
            dma((SEQS,)),
            dma,
            dma,
            dma((8,)), dma((16,)), dma((16,)), dma((8,)),
            dma((8,)), dma((16,)), dma((8,)), dma((8,)),
            dma((8,)), dma((16,)), dma((8,)), dma((8,)),
            dma((8,)), dma((4,)),
        ],
        compiler_params=pltpu.CompilerParams(collective_id=0, has_side_effects=True),
        name="decode",
    )(
        tokens, in_gain.reshape(1, 16), w_query, score_bias, cache_keys, cache_values, lengths,
        head_gain.reshape(1, DH), w_out.T,
    )


def solution(mesh):
    placed = (
        P(None, "kv"), P("kv"), P("kv", "tp"), P("tp"), P(None, "kv", "tp"), P(None, "kv", "tp"), P(), P("tp"),
        P("tp", "kv"),
    )
    return jax.shard_map(shards, mesh=mesh, in_specs=placed, out_specs=P(None, "kv"), check_vma=False)
```
